32 devices in a mesh: rep: 2 (over x), fs: 4 (over z), tp: 4 (over y, core).
Axes of the slice: x: 2, y: 2, z: 4, core: 2. Of those that a mesh axis runs over, the one named last changes fastest.
Arguments:
- tokens: bfloat16 [4096, 2048], P(('rep', 'fs', 'tp')), may hold values from -6 to 6
- mix_gain: float32 [2048], replicated, may hold values from 0.1 to 1.9
- w_query: bfloat16 [2048, 1024], P('fs', 'tp'), may hold values from -0.125 to 0.125
- w_key: bfloat16 [2048, 1024], P('fs', 'tp'), may hold values from -0.125 to 0.125
- w_value: bfloat16 [2048, 2048], P('fs', 'tp'), may hold values from -0.125 to 0.125
- w_decay_down: bfloat16 [2048, 32], replicated, may hold values from -0.125 to 0.125
- w_decay_up: bfloat16 [32, 1024], replicated, may hold values from -2 to 2
- decay_bias: float32 [1024], replicated, may hold values from -1 to 6
- decay_shift: float32 [4096, 1024], P(('rep', 'fs'), 'tp'), may hold values from -3 to 0
- head_gain: float32 [2048], replicated, may hold values from 0.1 to 1.9
- w_mix_out: bfloat16 [2048, 2048], P('tp', 'fs'), may hold values from -0.125 to 0.125
- ffn_gain: float32 [2048], replicated, may hold values from 0.1 to 1.9
- w_gate: bfloat16 [2048, 5632], P('fs', 'tp'), may hold values from -0.125 to 0.125
- w_up: bfloat16 [2048, 5632], P('fs', 'tp'), may hold values from -0.125 to 0.125
- w_down: bfloat16 [5632, 2048], P('tp', 'fs'), may hold values from -0.078125 to 0.078125
Outputs:
- layer_out: float32 [4096, 2048], P(('rep', 'fs', 'tp'))
The draws below stay inside these ranges and needn't reach their ends.
All inputs are finite; a program needn't handle non-finite values.
Results may differ from the reference program's by a relative error of at most 0.04.
Values may be sent and summed in bfloat16 or wider, within the bound.
No kernel may reach another device: no remote copies, remote signals or barrier semaphores. Data moves between devices by JAX's collectives and lax.ppermute only.
A program may use at most 128 MiB of HBM per device.

```python
import jax
import jax.numpy as jnp
from jax import lax

D = 2048
HEADS = 8
KEY_CHANNELS = 128
DV = 256
KEY = 1024
RANK = 32
FF = 5632
BLK = 64
SEQUENCE_LENGTH = 512
TOKENS = 4096
N_TP = 4


def draw_decay_bias(key, part):
    head_key, fast_key, slow_key = jax.random.split(key, 3)
    fast_chance = 0.5
    fast_heads = jax.random.bernoulli(head_key, fast_chance, (HEADS,))
    fast_values = jax.random.uniform(fast_key, (HEADS, KEY_CHANNELS), jnp.float32, -0.5, 1.5)
    slow_values = jax.random.uniform(slow_key, (HEADS, KEY_CHANNELS), jnp.float32, 4.0, 6.0)
    return jnp.where(fast_heads[:, None], fast_values, slow_values).reshape(KEY).astype(jnp.float32)


def draw_decay_shift(key, part):
    sequence_count = TOKENS // SEQUENCE_LENGTH
    location_key, depth_key, rate_key = jax.random.split(key, 3)
    spike_locations = jax.random.randint(location_key, (sequence_count, 3), 0, SEQUENCE_LENGTH)
    spike_magnitudes = jnp.log(jax.random.uniform(depth_key, (sequence_count, 3, HEADS), jnp.float32, 0.5, 0.8))
    row_ids = jnp.arange(TOKENS)
    sequence_index = row_ids // SEQUENCE_LENGTH
    token_positions = row_ids % SEQUENCE_LENGTH
    match_flags = (token_positions[:, None] == spike_locations[sequence_index]).astype(jnp.float32)
    spike_events = jnp.einsum('fi,fit->ft', match_flags, spike_magnitudes[sequence_index])
    block_count = TOKENS // BLK
    rates = -jnp.exp(jax.random.uniform(rate_key, (block_count, KEY), jnp.float32, jnp.log(0.3), jnp.log(3.0))) / SEQUENCE_LENGTH
    decay_rate_rows = jnp.repeat(rates, BLK, axis=0)
    return (jnp.repeat(spike_events, KEY_CHANNELS, axis=1) + decay_rate_rows).astype(jnp.float32)


def shard_levels(stream_key, dims, cuts, smallest, top_value):
    level, own = 1.0, jax.random.fold_in(stream_key, 6)
    for position, parts in cuts:
        heights = jnp.exp(jax.random.uniform(jax.random.fold_in(own, position), (parts,), jnp.float32, smallest / len(cuts), top_value / len(cuts)))
        level = level * jnp.repeat(heights, dims[position] // parts).reshape([-1 if axis == position else 1 for axis in range(len(dims))])
    return level


def scatter_about(stream_key, shape, spread, bound, cuts=(), dtype=jnp.bfloat16):
    drawn = spread * jax.random.normal(stream_key, shape, jnp.float32)
    if cuts:
        drawn = drawn * shard_levels(stream_key, shape, cuts, -0.22, 0.18)
    return jnp.clip(drawn, -bound, bound).astype(dtype)


def setup_inputs(seed: int = 0) -> dict:
    streams_of = jax.random.split(jax.random.key(seed), 16)
    return {
        "tokens": scatter_about(streams_of[0], (TOKENS, D), 1.0, 6.0, ((0, 32),)),
        "mix_gain": jnp.clip(1.0 + 0.18 * jax.random.normal(streams_of[1], (D,), jnp.float32), 0.1, 1.9),
        "w_query": scatter_about(streams_of[2], (D, KEY), D ** -0.5, 0.125, ((0, 4), (1, 4))),
        "w_key": scatter_about(streams_of[3], (D, KEY), D ** -0.5, 0.125, ((0, 4), (1, 4))),
        "w_value": scatter_about(streams_of[4], (D, D), D ** -0.5, 0.125, ((0, 4), (1, 4))),
        "w_decay_down": scatter_about(streams_of[5], (D, RANK), D ** -0.5, 0.125),
        "w_decay_up": scatter_about(streams_of[6], (RANK, KEY), (RANK // 4) ** -0.5, 2.0),
        "decay_bias": draw_decay_bias(jax.random.fold_in(streams_of[15], 71), 0),
        "decay_shift": draw_decay_shift(jax.random.fold_in(streams_of[15], 71), 0),
        "head_gain": jnp.clip(1.0 + 0.18 * jax.random.normal(streams_of[9], (D,), jnp.float32), 0.1, 1.9),
        "w_mix_out": scatter_about(streams_of[10], (D, D), D ** -0.5, 0.125, ((0, 4), (1, 4))),
        "ffn_gain": jnp.clip(1.0 + 0.18 * jax.random.normal(streams_of[11], (D,), jnp.float32), 0.1, 1.9),
        "w_gate": scatter_about(streams_of[12], (D, FF), D ** -0.5, 0.125, ((0, 4), (1, 4))),
        "w_up": scatter_about(streams_of[13], (D, FF), D ** -0.5, 0.125, ((0, 4), (1, 4))),
        "w_down": scatter_about(streams_of[14], (FF, D), FF ** -0.5, 0.078125, ((0, 4), (1, 4))),
    }


EPS = 1e-06
TAU = 16.0

def rms_norm(values, gain):
    return values * lax.rsqrt(lax.optimization_barrier(jnp.mean(values * values, axis=-1, keepdims=True)) + EPS) * gain

def recurrence(query_proj, key_proj, value_proj, log_decay):
    blocks = SEQUENCE_LENGTH // BLK
    queries = query_proj.astype(jnp.float32).reshape(blocks, BLK, HEADS, KEY_CHANNELS) * KEY_CHANNELS ** (-0.5)
    keys = key_proj.astype(jnp.float32).reshape(blocks, BLK, HEADS, KEY_CHANNELS)
    values = value_proj.astype(jnp.float32).reshape(blocks, BLK, HEADS, DV)
    decays = log_decay.reshape(blocks, BLK, HEADS, KEY_CHANNELS)
    cumul = jnp.cumsum(decays, axis=1)
    totals = cumul[:, -1]
    weighted = keys * jnp.exp(totals[:, None] - cumul)
    updates = jnp.einsum('bchd,bche->bhde', weighted, values, precision=lax.Precision.HIGHEST)

    def advance(state, inputs):
        total, update = inputs
        new_state = jnp.exp(total)[..., None] * state + update
        return (new_state, state)
    _, previous = lax.scan(advance, jnp.zeros((HEADS, KEY_CHANNELS, DV), jnp.float32), (totals, updates))
    q_decayed = queries * jnp.exp(cumul)
    k_decayed = keys * jnp.exp(-cumul)
    scores = jnp.einsum('bchd,bshd->bhcs', q_decayed, k_decayed, precision=lax.Precision.HIGHEST)
    causal = (jnp.arange(BLK)[:, None] >= jnp.arange(BLK)[None, :]).astype(jnp.float32)
    scores = scores * causal
    inner = jnp.einsum('bhcs,bshe->bche', scores, values, precision=lax.Precision.HIGHEST)
    carried = jnp.einsum('bchd,bhde->bche', q_decayed, previous, precision=lax.Precision.HIGHEST)
    return (inner + carried).reshape(SEQUENCE_LENGTH, HEADS, DV)

def reference(tokens, mix_gain, w_query, w_key, w_value, w_decay_down, w_decay_up, decay_bias, decay_shift, head_gain, w_mix_out, ffn_gain, w_gate, w_up, w_down):
    sequence_count = TOKENS // SEQUENCE_LENGTH
    out_groups = w_mix_out.astype(jnp.float32).reshape(N_TP, D // N_TP, D)
    down_groups = w_down.astype(jnp.float32).reshape(N_TP, FF // N_TP, D)

    def layer(inputs):
        seq_tokens, seq_shift = inputs
        source = seq_tokens.astype(jnp.float32)
        normed = rms_norm(source, mix_gain).astype(jnp.bfloat16)
        query_proj = jnp.dot(normed, w_query, preferred_element_type=jnp.float32).astype(jnp.bfloat16)
        key_proj = jnp.dot(normed, w_key, preferred_element_type=jnp.float32).astype(jnp.bfloat16)
        value_proj = jnp.dot(normed, w_value, preferred_element_type=jnp.float32).astype(jnp.bfloat16)
        low_rank = jnp.dot(normed, w_decay_down, preferred_element_type=jnp.float32).astype(jnp.bfloat16)
        pre_decay = jnp.dot(low_rank, w_decay_up, preferred_element_type=jnp.float32) + decay_bias
        log_decay = jax.nn.log_sigmoid(pre_decay) / TAU + seq_shift
        head_out = recurrence(query_proj, key_proj, value_proj, log_decay)
        gated = rms_norm(head_out, head_gain.reshape(HEADS, DV)).astype(jnp.bfloat16)
        gated = gated.reshape(SEQUENCE_LENGTH, N_TP, D // N_TP).astype(jnp.float32)
        partials = jnp.einsum('lgc,gcd->gld', gated, out_groups).astype(jnp.bfloat16)
        hidden = source + lax.optimization_barrier(jnp.sum(partials.astype(jnp.float32), axis=0))
        normed_ffn = rms_norm(hidden, ffn_gain).astype(jnp.bfloat16)
        gate_proj = jnp.dot(normed_ffn, w_gate, preferred_element_type=jnp.float32)
        up_proj = jnp.dot(normed_ffn, w_up, preferred_element_type=jnp.float32)
        activated = (jax.nn.silu(gate_proj) * up_proj).astype(jnp.bfloat16)
        activated = activated.reshape(SEQUENCE_LENGTH, N_TP, FF // N_TP).astype(jnp.float32)
        ffn_parts = jnp.einsum('lgc,gcd->gld', activated, down_groups).astype(jnp.bfloat16)
        return hidden + lax.optimization_barrier(jnp.sum(ffn_parts.astype(jnp.float32), axis=0))
    result = lax.map(layer, (tokens.reshape(sequence_count, SEQUENCE_LENGTH, D), decay_shift.reshape(sequence_count, SEQUENCE_LENGTH, KEY)))
    return result.reshape(TOKENS, D)
```

```python
import functools

import jax
import jax.numpy as jnp
from jax import lax
from jax.experimental import pallas as pl
from jax.experimental.pallas import tpu as pltpu
from jax.sharding import PartitionSpec as P

KEY_CHANNELS = 128
DV = 256
BLK = 64


EPS = 1e-06
TAU = 16.0


def rms_norm(values, gain):
    return values * lax.rsqrt(jnp.mean(values * values, axis=-1, keepdims=True) + EPS) * gain


def recurrence(query_proj, key_proj, value_proj, log_decay, head_count):
    seq_rows = query_proj.shape[0]
    blocks = seq_rows // BLK
    queries = query_proj.astype(jnp.float32).reshape(
        blocks, BLK, head_count, KEY_CHANNELS
    ) * KEY_CHANNELS ** (-0.5)
    keys = key_proj.astype(jnp.float32).reshape(blocks, BLK, head_count, KEY_CHANNELS)
    values = value_proj.astype(jnp.float32).reshape(blocks, BLK, head_count, DV)
    decays = log_decay.reshape(blocks, BLK, head_count, KEY_CHANNELS)
    cumul = jnp.cumsum(decays, axis=1)
    totals = cumul[:, -1]
    weighted = keys * jnp.exp(totals[:, None] - cumul)
    updates = jnp.einsum("bchd,bche->bhde", weighted, values, precision=lax.Precision.HIGHEST)

    def combine(earlier, later):
        return (earlier[0] + later[0], jnp.exp(later[0])[..., None] * earlier[1] + later[1])

    _, states = lax.associative_scan(combine, (totals, updates), axis=0)
    previous = jnp.concatenate([jnp.zeros_like(states[:1]), states[:-1]], axis=0)
    q_decayed = queries * jnp.exp(cumul)
    k_decayed = keys * jnp.exp(-cumul)
    scores = jnp.einsum("bchd,bshd->bhcs", q_decayed, k_decayed, precision=lax.Precision.HIGHEST)
    causal = (jnp.arange(BLK)[:, None] >= jnp.arange(BLK)[None, :]).astype(jnp.float32)
    scores = scores * causal
    inner = jnp.einsum("bhcs,bshe->bche", scores, values, precision=lax.Precision.HIGHEST)
    carried = jnp.einsum("bchd,bhde->bche", q_decayed, previous, precision=lax.Precision.HIGHEST)
    return (inner + carried).reshape(seq_rows, head_count, DV)


def plain_device(
    tokens,
    mix_gain,
    w_query,
    w_key,
    w_value,
    w_decay_down,
    w_decay_up,
    decay_bias,
    decay_shift,
    head_gain,
    w_mix_out,
    ffn_gain,
    w_gate,
    w_up,
    w_down,
):
    tp_index = lax.axis_index("tp")
    own_count = tokens.shape[0]
    key_cols = w_query.shape[1]
    value_cols = w_value.shape[1]
    heads_dev = key_cols // KEY_CHANNELS
    whole_input = lax.all_gather(tokens, "tp", axis=0, tiled=True).astype(jnp.float32)
    normed = rms_norm(whole_input, mix_gain).astype(jnp.bfloat16)
    seq_rows = normed.shape[0]
    pieces = (
        lax.all_gather(w_query, "fs", axis=0, tiled=True),
        lax.all_gather(w_key, "fs", axis=0, tiled=True),
        lax.all_gather(w_value, "fs", axis=0, tiled=True),
    )
    first = jnp.dot(normed, pieces[0], preferred_element_type=jnp.float32)
    second = jnp.dot(normed, pieces[1], preferred_element_type=jnp.float32)
    third = jnp.dot(normed, pieces[2], preferred_element_type=jnp.float32)
    query_proj = first.astype(jnp.bfloat16)
    key_proj = second.astype(jnp.bfloat16)
    value_proj = third.astype(jnp.bfloat16)
    low_rank = jnp.dot(normed, w_decay_down, preferred_element_type=jnp.float32).astype(
        jnp.bfloat16
    )
    up_columns = lax.dynamic_slice_in_dim(w_decay_up, tp_index * key_cols, key_cols, 1)
    bias_columns = lax.dynamic_slice_in_dim(decay_bias, tp_index * key_cols, key_cols, 0)
    pre_decay = jnp.dot(low_rank, up_columns, preferred_element_type=jnp.float32) + bias_columns
    log_decay = jax.nn.log_sigmoid(pre_decay) / TAU + decay_shift
    head_out = recurrence(query_proj, key_proj, value_proj, log_decay, heads_dev)
    gain_columns = lax.dynamic_slice_in_dim(head_gain, tp_index * value_cols, value_cols, 0)
    gated = rms_norm(head_out, gain_columns.reshape(heads_dev, DV)).astype(jnp.bfloat16)
    gated = gated.reshape(seq_rows, value_cols)
    out_weight = lax.all_gather(w_mix_out, "fs", axis=1, tiled=True)
    mixer_full = lax.psum(
        jnp.dot(gated, out_weight, preferred_element_type=jnp.float32).astype(jnp.bfloat16), "tp"
    ).astype(jnp.float32)
    hidden_all = whole_input + mixer_full
    normed_ffn = rms_norm(hidden_all, ffn_gain).astype(jnp.bfloat16)
    hidden = lax.dynamic_slice_in_dim(hidden_all, tp_index * own_count, own_count, 0)

    def add_single(piece):
        return jnp.dot(normed_ffn, piece, preferred_element_type=jnp.float32)

    pieces = (
        lax.all_gather(w_gate, "fs", axis=0, tiled=True),
        lax.all_gather(w_up, "fs", axis=0, tiled=True),
    )
    gate_proj = add_single(pieces[0])
    up_proj = add_single(pieces[1])
    activated = (jax.nn.silu(gate_proj) * up_proj).astype(jnp.bfloat16)
    down_weight = lax.all_gather(w_down, "fs", axis=1, tiled=True)
    return hidden + lax.psum_scatter(
        jnp.dot(activated, down_weight, preferred_element_type=jnp.float32).astype(jnp.bfloat16),
        "tp",
        scatter_dimension=0,
        tiled=True,
    ).astype(jnp.float32)


LANES = 128
F32 = jnp.float32
BF16 = jnp.bfloat16
VMEM = pl.BlockSpec(memory_space=pltpu.VMEM)
SMEM = pl.BlockSpec(memory_space=pltpu.SMEM)
PLANE = ("rep", "tp")


def dot(a, b, dims=((1,), (0,))):
    return lax.dot_general(a, b, (dims, ((), ())), preferred_element_type=F32)


def parts(value):
    high = value.astype(BF16)
    return high, (value - high.astype(F32)).astype(BF16)


def fine_dot(a, b, dims=((1,), (0,))):
    left = (a,) if a.dtype == BF16 else parts(a)
    right = (b,) if b.dtype == BF16 else parts(b)
    total = dot(left[0], right[0], dims)
    if len(right) > 1:
        total = total + dot(left[0], right[1], dims)
    if len(left) > 1:
        total = total + dot(left[1], right[0], dims)
    return total


def swap(value, mask, count):
    return lax.ppermute(value, PLANE, [(i, i ^ mask) for i in range(count)])


def plane_gather(own, count):
    pieces = [own] + [None] * (count - 1)
    for mask in (1, 4, 2, 6):
        pieces[mask] = swap(own, mask, count)
    for mask in (4, 2, 6):
        pieces[mask + 1] = swap(pieces[mask], 1, count)
    return pieces


def plane_reduce(even, odd, count):
    other = swap(odd, 1, count)
    both = even.astype(F32) + other.astype(F32)
    sent = both[1:].astype(BF16)
    total = both[0]
    for place, mask in enumerate((2, 4, 6)):
        total = total + swap(sent[place], mask, count).astype(F32)
    return total


def line_gather(own):
    size = lax.axis_size("fs")
    two = lax.ppermute(own, "fs", [(i, i ^ 2) for i in range(size)])
    below = lax.ppermute(own, "fs", [(i, i + 1) for i in range(size - 1)])
    above = lax.ppermute(own, "fs", [(i + 1, i) for i in range(size - 1)])
    return below, two, above


def line_forward(two):
    return lax.ppermute(two, "fs", [(2, 3), (1, 0)])


def rotate(value, axis):
    size = lax.axis_size("fs")
    block = value.shape[axis] // size
    index = lax.axis_index("fs")
    order = [lax.rem(index - k + size, size) for k in range(size)]
    return jnp.concatenate(
        [lax.dynamic_slice_in_dim(value, place * block, block, axis) for place in order], axis
    )


def attention_kernel(
    scal, *refs, rows, channels, values, blocks
):
    tok = refs[:8]
    (gain, own_w, below, two, above, fourth, down_w, up_w, bias, shift_own, shift_other, hgain) = refs[8:20]
    gated_out = refs[20]
    proj, logd = refs[21:]
    at = scal[0]
    place = scal[1]
    first, last = at == 0, at == 3
    part = own_w.shape[0]
    width = own_w.shape[1]
    weight = [
        own_w[...],
        jnp.where(first, fourth[...], below[...]),
        two[...],
        jnp.where(last, fourth[...], above[...]),
    ]
    for m in range(8):
        source = tok[m][...].astype(F32)
        scale = lax.rsqrt(jnp.mean(source * source, axis=-1, keepdims=True) + EPS)
        normed = (source * scale * gain[...]).astype(BF16)
        total = dot(normed[:, :part], weight[0])
        for k in range(1, 4):
            total = total + dot(normed[:, k * part : (k + 1) * part], weight[k])
        proj[m * rows : (m + 1) * rows, :] = total.astype(BF16)
        low = dot(normed, down_w[...]).astype(BF16)
        pre = dot(low, up_w[...]) + bias[...]
        logd[m * rows : (m + 1) * rows, :] = jax.nn.log_sigmoid(pre) / TAU
    tri_row = lax.broadcasted_iota(jnp.int32, (BLK, BLK), 0)
    tri_col = lax.broadcasted_iota(jnp.int32, (BLK, BLK), 1)
    tri = (tri_row >= tri_col).astype(F32)
    per = rows // BLK
    for seq in range(2):
        shift = (shift_own, shift_other)[seq]
        state = jnp.zeros((values, channels), F32)
        for b in range(blocks):
            m = seq * 4 + ((b // per) ^ place)
            offset = pl.multiple_of(m * rows + (b % per) * BLK, BLK)
            decay = logd[pl.ds(offset, BLK), :] + shift[b * BLK : (b + 1) * BLK, :]
            cum = lax.dot_general(
                tri, decay, (((1,), (0,)), ((), ())),
                precision=lax.Precision.HIGHEST, preferred_element_type=F32,
            )
            tot = cum[BLK - 1 :, :]
            q = proj[pl.ds(offset, BLK), :channels].astype(F32) * channels ** (-0.5)
            k = proj[pl.ds(offset, BLK), channels : 2 * channels].astype(F32)
            v = proj[pl.ds(offset, BLK), 2 * channels :]
            qd = q * jnp.exp(cum)
            kd = k * jnp.exp(-cum)
            kw = k * jnp.exp(tot - cum)
            scores = lax.dot_general(
                qd, kd, (((1,), (1,)), ((), ())),
                precision=lax.Precision.HIGHEST, preferred_element_type=F32,
            )
            scores = scores * tri
            out = fine_dot(scores, v)
            if b:
                out = out + fine_dot(qd, state, ((1,), (1,)))
            scale = lax.rsqrt(jnp.mean(out * out, axis=-1, keepdims=True) + EPS)
            gated_out[pl.ds(offset, BLK), :] = (out * scale * hgain[...]).astype(BF16)
            if b + 1 < blocks:
                state = jnp.exp(tot) * state + fine_dot(v, kw, ((0,), (0,)))


def mix_kernel(scal, value, own_w, below, two, above, fourth, even, odd, *, rows):
    at = scal[0]
    part = own_w.shape[1]
    weight = [
        own_w[...],
        jnp.where(at == 0, fourth[...], below[...]),
        two[...],
        jnp.where(at == 3, fourth[...], above[...]),
    ]
    for m in range(8):
        left = value[m * rows : (m + 1) * rows, :]
        out = (even, odd)[m % 2]
        for k in range(4):
            out[m // 2, :, k * part : (k + 1) * part] = dot(left, weight[k]).astype(BF16)


def gate_kernel(scal, *refs, rows, main):
    pieces = refs[:8]
    own_w, below, two, above, fourth, act = refs[8:]
    at = scal[0]
    part = own_w.shape[0]
    weight = [
        own_w[...],
        jnp.where(at == 0, fourth[...], below[...]),
        two[...],
        jnp.where(at == 3, fourth[...], above[...]),
    ]
    tail = own_w.shape[1] // 2 - main
    for m in range(8):
        total = dot(pieces[m][:, :part], weight[0])
        for k in range(1, 4):
            total = total + dot(pieces[m][:, k * part : (k + 1) * part], weight[k])
        place = slice(m * rows, (m + 1) * rows)
        act[place, :main] = (jax.nn.silu(total[:, :main]) * total[:, main : 2 * main]).astype(BF16)
        if tail:
            gate = total[:, 2 * main : 2 * main + tail]
            act[place, main:] = (jax.nn.silu(gate) * total[:, 2 * main + tail :]).astype(BF16)


def call(kernel, outs, *args, scratch=(), **static):
    return pl.pallas_call(
        functools.partial(kernel, **static),
        out_shape=outs,
        in_specs=[SMEM] + [VMEM] * (len(args) - 1),
        out_specs=jax.tree.map(lambda _: VMEM, outs),
        scratch_shapes=scratch,
        compiler_params=pltpu.CompilerParams(vmem_limit_bytes=60 * 1024 * 1024),
    )(*args)


def split_device(
    tokens,
    mix_gain,
    w_query,
    w_key,
    w_value,
    w_decay_down,
    w_decay_up,
    decay_bias,
    decay_shift,
    head_gain,
    w_mix_out,
    ffn_gain,
    w_gate,
    w_up,
    w_down,
):
    rep, at, tp = (lax.axis_index(name) for name in ("rep", "fs", "tp"))
    reps = lax.axis_size("rep")
    count = reps * lax.axis_size("tp")
    rows, width = tokens.shape
    low = rep == 0
    keys, vals = w_query.shape[1] // reps, w_value.shape[1] // reps
    units = w_gate.shape[1] // reps
    main = units // LANES * LANES
    scal = jnp.stack([at, tp]).astype(jnp.int32)

    def side(value, own=True):
        half = value.shape[1] // 2
        pick = low if own else jnp.logical_not(low)
        return jnp.where(pick, value[:, :half], value[:, half:])

    own_tok = rotate(tokens, 1)
    tok = plane_gather(own_tok, count)
    shift_other = swap(side(decay_shift, False), lax.axis_size("tp"), count)
    w_qkv = jnp.concatenate([side(w_query), side(w_key), side(w_value)], axis=1)
    qkv = line_gather(w_qkv)
    w_mix = lax.dynamic_slice_in_dim(w_mix_out, rep * vals, vals, 0)
    mix = line_gather(w_mix)
    qkv_end = line_forward(qkv[1])
    mix_end = line_forward(mix[1])

    def unit_cols(value):
        far = value.shape[1] - main
        return (
            jnp.where(low, value[:, :main], value[:, far:]),
            jnp.where(low, value[:, main:units], value[:, units:far]) if units > main else value[:, :0],
        )

    gate_main, gate_tail = unit_cols(w_gate)
    up_main, up_tail = unit_cols(w_up)
    w_gu = jnp.concatenate([gate_main, up_main, gate_tail, up_tail], axis=1)
    far = w_down.shape[0] - main
    w_dn = jnp.concatenate(
        [
            jnp.where(low, w_down[:main], w_down[far:]),
            jnp.where(low, w_down[main:units], w_down[units:far]),
        ],
        axis=0,
    )
    w_gu, w_dn, _ = lax.optimization_barrier((w_gu, w_dn, mix[1][:8]))
    gu = line_gather(w_gu)
    gu_end = line_forward(gu[1])
    dn = line_gather(w_dn)
    dn_end = line_forward(dn[1])

    head = (tp * reps + rep) * keys
    up_cols = lax.dynamic_slice_in_dim(w_decay_up, head, keys, 1)
    bias = lax.dynamic_slice_in_dim(decay_bias, head, keys, 0).reshape(1, keys)
    hgain = lax.dynamic_slice_in_dim(head_gain, (tp * reps + rep) * vals, vals, 0).reshape(1, vals)
    gain_mix = rotate(mix_gain.reshape(1, width), 1)
    gain_ffn = rotate(ffn_gain.reshape(1, width), 1)
    down_cols = rotate(w_decay_down, 0)

    gated = call(
        attention_kernel,
        jax.ShapeDtypeStruct((count * rows, vals), BF16),
        scal, *tok, gain_mix, w_qkv, *qkv, qkv_end, down_cols, up_cols, bias,
        side(decay_shift), shift_other, hgain,
        scratch=(
            pltpu.VMEM((count * rows, 2 * keys + vals), BF16),
            pltpu.VMEM((count * rows, keys), F32),
        ),
        rows=rows, channels=keys, values=vals, blocks=decay_shift.shape[0] // BLK,
    )
    halves = [jax.ShapeDtypeStruct((count // 2, rows, width), BF16)] * 2
    even, odd = call(mix_kernel, halves, scal, gated, w_mix, *mix, mix_end, rows=rows)
    hidden = own_tok.astype(F32) + plane_reduce(even, odd, count)
    normed = rms_norm(hidden, gain_ffn).astype(BF16)
    pieces = plane_gather(normed, count)
    act = call(
        gate_kernel,
        jax.ShapeDtypeStruct((count * rows, units), BF16),
        scal, *pieces, w_gu, *gu, gu_end, rows=rows, main=main,
    )
    even, odd = call(mix_kernel, halves, scal, act, w_dn, *dn, dn_end, rows=rows)
    return rotate(hidden + plane_reduce(even, odd, count), 1)


def solution(mesh):
    sizes = dict(mesh.shape)
    fits = sizes["rep"] == 2 and sizes["fs"] == 4 and sizes["tp"] == 4
    per_device = split_device if fits else plain_device
    return jax.shard_map(
        per_device,
        mesh=mesh,
        in_specs=(
            P(("rep", "fs", "tp"), None),
            P(),
            P("fs", "tp"),
            P("fs", "tp"),
            P("fs", "tp"),
            P(),
            P(),
            P(),
            P(("rep", "fs"), "tp"),
            P(),
            P("tp", "fs"),
            P(),
            P("fs", "tp"),
            P("fs", "tp"),
            P("tp", "fs"),
        ),
        out_specs=P(("rep", "fs", "tp"), None),
        check_vma=False,
    )
```

```python
import functools

import jax
import jax.numpy as jnp
from jax import lax
from jax.experimental import pallas as pl
from jax.experimental.pallas import tpu as pltpu
from jax.sharding import PartitionSpec as P

KEY_CHANNELS = 128
DV = 256
BLK = 64


EPS = 1e-06
TAU = 16.0


def rms_norm(values, gain):
    return values * lax.rsqrt(jnp.mean(values * values, axis=-1, keepdims=True) + EPS) * gain


def recurrence(query_proj, key_proj, value_proj, log_decay, head_count):
    seq_rows = query_proj.shape[0]
    blocks = seq_rows // BLK
    queries = query_proj.astype(jnp.float32).reshape(
        blocks, BLK, head_count, KEY_CHANNELS
    ) * KEY_CHANNELS ** (-0.5)
    keys = key_proj.astype(jnp.float32).reshape(blocks, BLK, head_count, KEY_CHANNELS)
    values = value_proj.astype(jnp.float32).reshape(blocks, BLK, head_count, DV)
    decays = log_decay.reshape(blocks, BLK, head_count, KEY_CHANNELS)
    cumul = jnp.cumsum(decays, axis=1)
    totals = cumul[:, -1]
    weighted = keys * jnp.exp(totals[:, None] - cumul)
    updates = jnp.einsum("bchd,bche->bhde", weighted, values, precision=lax.Precision.HIGHEST)

    def combine(earlier, later):
        return (earlier[0] + later[0], jnp.exp(later[0])[..., None] * earlier[1] + later[1])

    _, states = lax.associative_scan(combine, (totals, updates), axis=0)
    previous = jnp.concatenate([jnp.zeros_like(states[:1]), states[:-1]], axis=0)
    q_decayed = queries * jnp.exp(cumul)
    k_decayed = keys * jnp.exp(-cumul)
    scores = jnp.einsum("bchd,bshd->bhcs", q_decayed, k_decayed, precision=lax.Precision.HIGHEST)
    causal = (jnp.arange(BLK)[:, None] >= jnp.arange(BLK)[None, :]).astype(jnp.float32)
    scores = scores * causal
    inner = jnp.einsum("bhcs,bshe->bche", scores, values, precision=lax.Precision.HIGHEST)
    carried = jnp.einsum("bchd,bhde->bche", q_decayed, previous, precision=lax.Precision.HIGHEST)
    return (inner + carried).reshape(seq_rows, head_count, DV)


def plain_device(
    tokens,
    mix_gain,
    w_query,
    w_key,
    w_value,
    w_decay_down,
    w_decay_up,
    decay_bias,
    decay_shift,
    head_gain,
    w_mix_out,
    ffn_gain,
    w_gate,
    w_up,
    w_down,
):
    tp_index = lax.axis_index("tp")
    own_count = tokens.shape[0]
    key_cols = w_query.shape[1]
    value_cols = w_value.shape[1]
    heads_dev = key_cols // KEY_CHANNELS
    whole_input = lax.all_gather(tokens, "tp", axis=0, tiled=True).astype(jnp.float32)
    normed = rms_norm(whole_input, mix_gain).astype(jnp.bfloat16)
    seq_rows = normed.shape[0]
    pieces = (
        lax.all_gather(w_query, "fs", axis=0, tiled=True),
        lax.all_gather(w_key, "fs", axis=0, tiled=True),
        lax.all_gather(w_value, "fs", axis=0, tiled=True),
    )
    first = jnp.dot(normed, pieces[0], preferred_element_type=jnp.float32)
    second = jnp.dot(normed, pieces[1], preferred_element_type=jnp.float32)
    third = jnp.dot(normed, pieces[2], preferred_element_type=jnp.float32)
    query_proj = first.astype(jnp.bfloat16)
    key_proj = second.astype(jnp.bfloat16)
    value_proj = third.astype(jnp.bfloat16)
    low_rank = jnp.dot(normed, w_decay_down, preferred_element_type=jnp.float32).astype(
        jnp.bfloat16
    )
    up_columns = lax.dynamic_slice_in_dim(w_decay_up, tp_index * key_cols, key_cols, 1)
    bias_columns = lax.dynamic_slice_in_dim(decay_bias, tp_index * key_cols, key_cols, 0)
    pre_decay = jnp.dot(low_rank, up_columns, preferred_element_type=jnp.float32) + bias_columns
    log_decay = jax.nn.log_sigmoid(pre_decay) / TAU + decay_shift
    head_out = recurrence(query_proj, key_proj, value_proj, log_decay, heads_dev)
    gain_columns = lax.dynamic_slice_in_dim(head_gain, tp_index * value_cols, value_cols, 0)
    gated = rms_norm(head_out, gain_columns.reshape(heads_dev, DV)).astype(jnp.bfloat16)
    gated = gated.reshape(seq_rows, value_cols)
    out_weight = lax.all_gather(w_mix_out, "fs", axis=1, tiled=True)
    mixer_full = lax.psum(
        jnp.dot(gated, out_weight, preferred_element_type=jnp.float32).astype(jnp.bfloat16), "tp"
    ).astype(jnp.float32)
    hidden_all = whole_input + mixer_full
    normed_ffn = rms_norm(hidden_all, ffn_gain).astype(jnp.bfloat16)
    hidden = lax.dynamic_slice_in_dim(hidden_all, tp_index * own_count, own_count, 0)

    def add_single(piece):
        return jnp.dot(normed_ffn, piece, preferred_element_type=jnp.float32)

    pieces = (
        lax.all_gather(w_gate, "fs", axis=0, tiled=True),
        lax.all_gather(w_up, "fs", axis=0, tiled=True),
    )
    gate_proj = add_single(pieces[0])
    up_proj = add_single(pieces[1])
    activated = (jax.nn.silu(gate_proj) * up_proj).astype(jnp.bfloat16)
    down_weight = lax.all_gather(w_down, "fs", axis=1, tiled=True)
    return hidden + lax.psum_scatter(
        jnp.dot(activated, down_weight, preferred_element_type=jnp.float32).astype(jnp.bfloat16),
        "tp",
        scatter_dimension=0,
        tiled=True,
    ).astype(jnp.float32)


LANES = 128
F32 = jnp.float32
BF16 = jnp.bfloat16
VMEM = pl.BlockSpec(memory_space=pltpu.VMEM)
SMEM = pl.BlockSpec(memory_space=pltpu.SMEM)
PLANE = ("rep", "tp")


def dot(a, b, dims=((1,), (0,))):
    return lax.dot_general(a, b, (dims, ((), ())), preferred_element_type=F32)


def parts(value):
    high = value.astype(BF16)
    return high, (value - high.astype(F32)).astype(BF16)


def fine_dot(a, b, dims=((1,), (0,))):
    left = (a,) if a.dtype == BF16 else parts(a)
    right = (b,) if b.dtype == BF16 else parts(b)
    total = dot(left[0], right[0], dims)
    if len(right) > 1:
        total = total + dot(left[0], right[1], dims)
    if len(left) > 1:
        total = total + dot(left[1], right[0], dims)
    return total


def swap(value, mask, count):
    return lax.ppermute(value, PLANE, [(i, i ^ mask) for i in range(count)])


def plane_gather(own, count, before=()):
    pieces = [own] + [None] * (count - 1)
    for mask in (4, 2, 6, 1):
        pieces[mask] = swap(own, mask, count)
    if before:
        pieces[6], *before = lax.optimization_barrier((pieces[6], *before))
    for mask in (4, 2, 6):
        pieces[mask + 1] = swap(pieces[mask], 1, count)
    return pieces, before


def plane_reduce(even, odd, count):
    other = swap(odd, 1, count)
    sums = [even[0].astype(F32) + other[0].astype(F32)]
    sent = {
        mask: (even[mask // 2].astype(F32) + other[mask // 2].astype(F32)).astype(BF16)
        for mask in (4, 2, 6)
    }
    return sums + [swap(sent[mask], mask, count) for mask in (6, 4, 2)]


def line_near(own):
    size = lax.axis_size("fs")
    return lax.ppermute(own, "fs", [(i, i ^ 1) for i in range(size)])


def line_far(own):
    size = lax.axis_size("fs")
    two = lax.ppermute(own, "fs", [(i, i ^ 2) for i in range(size)])
    inner = lax.ppermute(own, "fs", [(1, 2), (2, 1)])
    return two, inner


def line_gather(own):
    two, inner = line_far(own)
    return line_near(own), two, inner


def line_forward(two, both=True):
    size = lax.axis_size("fs")
    pairs = [(i, i ^ 1) for i in range(size)] if both else [(1, 0), (2, 3)]
    return lax.ppermute(two, "fs", pairs)


def rotate(value, axis):
    size = lax.axis_size("fs")
    block = value.shape[axis] // size
    index = lax.axis_index("fs")
    order = [index ^ k for k in range(size)]
    return jnp.concatenate(
        [lax.dynamic_slice_in_dim(value, place * block, block, axis) for place in order], axis
    )


def pick_late(scal, inner, fourth):
    at = scal[0]
    return jnp.where(jnp.logical_or(at == 0, at == 3), fourth[...], inner[...])


def pick_weights(scal, own_w, near, two, inner, fourth):
    return [own_w[...], near[...], two[...], pick_late(scal, inner, fourth)]


def project_kernel(scal, *refs, rows):
    tok = refs[:8]
    gain, own_w, near, two, inner, fourth, down_w, up_w, bias, proj, logd = refs[8:]
    weight = pick_weights(scal, own_w, near, two, inner, fourth)
    part = own_w.shape[0]
    for m in range(8):
        source = tok[m][...].astype(F32)
        scale = lax.rsqrt(jnp.mean(source * source, axis=-1, keepdims=True) + EPS)
        normed = (source * scale * gain[...]).astype(BF16)
        total = dot(normed[:, :part], weight[0])
        for k in range(1, 4):
            total = total + dot(normed[:, k * part : (k + 1) * part], weight[k])
        proj[m * rows : (m + 1) * rows, :] = total.astype(BF16)
        low = dot(normed, down_w[...]).astype(BF16)
        pre = dot(low, up_w[...]) + bias[...]
        logd[m * rows : (m + 1) * rows, :] = jax.nn.log_sigmoid(pre) / TAU


def recurrence_kernel(
    scal, proj, logd, shift_own, shift_other, hgain, gated_out, *, rows, channels, values, blocks
):
    place = scal[1]
    tri_row = lax.broadcasted_iota(jnp.int32, (BLK, BLK), 0)
    tri_col = lax.broadcasted_iota(jnp.int32, (BLK, BLK), 1)
    tri = (tri_row >= tri_col).astype(F32)
    per = rows // BLK
    states = [None, None]
    for b in range(blocks):
        for seq in range(2):
            shift = (shift_own, shift_other)[seq]
            m = seq * 4 + ((b // per) ^ place)
            offset = pl.multiple_of(m * rows + (b % per) * BLK, BLK)
            decay = logd[pl.ds(offset, BLK), :] + shift[b * BLK : (b + 1) * BLK, :]
            cum = lax.dot_general(
                tri, decay, (((1,), (0,)), ((), ())),
                precision=lax.Precision.HIGHEST, preferred_element_type=F32,
            )
            tot = cum[BLK - 1 :, :]
            q = proj[pl.ds(offset, BLK), :channels].astype(F32) * channels ** (-0.5)
            k = proj[pl.ds(offset, BLK), channels : 2 * channels].astype(F32)
            v = proj[pl.ds(offset, BLK), 2 * channels :]
            qd = q * jnp.exp(cum)
            kd = k * jnp.exp(-cum)
            scores = lax.dot_general(
                qd, kd, (((1,), (1,)), ((), ())),
                precision=lax.Precision.HIGHEST, preferred_element_type=F32,
            )
            out = fine_dot(scores * tri, v)
            if b:
                out = out + fine_dot(qd, states[seq], ((1,), (1,)))
            scale = lax.rsqrt(jnp.mean(out * out, axis=-1, keepdims=True) + EPS)
            gated_out[pl.ds(offset, BLK), :] = (out * scale * hgain[...]).astype(BF16)
            if b + 1 < blocks:
                update = fine_dot(v, k * jnp.exp(tot - cum), ((0,), (0,)))
                states[seq] = jnp.exp(tot) * states[seq] + update if b else update


def store_blocks(value, weights, even, odd, rows):
    for m in range(8):
        left = value[m * rows : (m + 1) * rows, :]
        out = (even, odd)[m % 2]
        start = 0
        for weight in weights:
            size = weight.shape[1]
            out[m // 2, :, start : start + size] = dot(left, weight).astype(BF16)
            start += size


def mix_kernel(scal, value, own_w, near, two, inner, fourth, even, odd, *, rows):
    store_blocks(value, pick_weights(scal, own_w, near, two, inner, fourth), even, odd, rows)


def columns_kernel(scal, value, *refs, rows):
    *weights, even, odd = refs
    store_blocks(value, [weight[...] for weight in weights], even, odd, rows)


def second_kernel(scal, value, inner, fourth, even, odd, *, rows):
    store_blocks(value, [pick_late(scal, inner, fourth)], even, odd, rows)


def gate_first_kernel(scal, *refs, rows):
    pieces = refs[:8]
    own_w, near, two, total = refs[8:]
    part = own_w.shape[0]
    for m in range(8):
        value = dot(pieces[m][:, :part], own_w[...])
        value = value + dot(pieces[m][:, part : 2 * part], near[...])
        value = value + dot(pieces[m][:, 2 * part : 3 * part], two[...])
        total[m * rows : (m + 1) * rows, :] = value


def gate_second_kernel(scal, *refs, rows, main):
    pieces = refs[:8]
    partial, inner, fourth, act = refs[8:]
    weight = pick_late(scal, inner, fourth)
    part = weight.shape[0]
    tail = weight.shape[1] // 2 - main
    for m in range(8):
        place = slice(m * rows, (m + 1) * rows)
        total = partial[place, :] + dot(pieces[m][:, 3 * part :], weight)
        act[place, :main] = (jax.nn.silu(total[:, :main]) * total[:, main : 2 * main]).astype(BF16)
        if tail:
            gate = total[:, 2 * main : 2 * main + tail]
            act[place, main:] = (jax.nn.silu(gate) * total[:, 2 * main + tail :]).astype(BF16)


def pack_kernel(scal, query, key, value, out):
    start = 0
    for ref in (query, key, value):
        size = ref.shape[1] // 2
        from_col = pl.multiple_of(scal[2] * size, LANES)
        out[:, start : start + size] = ref[:, pl.ds(from_col, size)]
        start += size


def merge_kernel(scal, hidden, *refs, part):
    *groups, out = refs
    at = scal[0]
    half = part // 2
    place = {0: [(0, 0, part)], 1: [(0, part, half), (1, part, half)], 2: [(1, 0, part)], 3: []}
    for k, pieces in place.items():
        total = hidden[:, k * part : (k + 1) * part]
        if pieces:
            total = total + jnp.concatenate(
                [
                    sum(ref[:, col : col + size].astype(F32) for ref in groups[4 * g : 4 * g + 4])
                    for g, col, size in pieces
                ],
                axis=1,
            )
        out[:, pl.ds(pl.multiple_of((at ^ k) * part, part), part)] = total


def last_kernel(scal, total, *refs):
    *group, out = refs
    value = total[...]
    for ref in group:
        value = value + ref[...].astype(F32)
    out[...] = value


def add_last(scal, total, group):
    rows, part = group[0].shape
    block = pl.BlockSpec((rows, part), lambda i, scal: (0, scal[0] ^ 3))
    whole = pl.BlockSpec((rows, part), lambda i, scal: (0, 0))
    return pl.pallas_call(
        last_kernel,
        out_shape=jax.ShapeDtypeStruct(total.shape, total.dtype),
        grid_spec=pltpu.PrefetchScalarGridSpec(
            num_scalar_prefetch=1,
            grid=(1,),
            in_specs=[block] + [whole] * len(group),
            out_specs=block,
        ),
        input_output_aliases={1: 0},
    )(scal, total, *group)


def call(kernel, outs, *args, **static):
    return pl.pallas_call(
        functools.partial(kernel, **static),
        out_shape=outs,
        in_specs=[SMEM] + [VMEM] * (len(args) - 1),
        out_specs=jax.tree.map(lambda _: VMEM, outs),
        compiler_params=pltpu.CompilerParams(vmem_limit_bytes=60 * 1024 * 1024),
    )(*args)


def split_device(
    tokens,
    mix_gain,
    w_query,
    w_key,
    w_value,
    w_decay_down,
    w_decay_up,
    decay_bias,
    decay_shift,
    head_gain,
    w_mix_out,
    ffn_gain,
    w_gate,
    w_up,
    w_down,
):
    rep, at, tp = (lax.axis_index(name) for name in ("rep", "fs", "tp"))
    reps = lax.axis_size("rep")
    count = reps * lax.axis_size("tp")
    rows, width = tokens.shape
    low = rep == 0
    keys, vals = w_query.shape[1] // reps, w_value.shape[1] // reps
    units = w_gate.shape[1] // reps
    main = units // LANES * LANES
    scal = jnp.stack([at, tp, rep]).astype(jnp.int32)

    def side(value, own=True):
        half = value.shape[1] // 2
        pick = low if own else jnp.logical_not(low)
        return jnp.where(pick, value[:, :half], value[:, half:])

    own_tok = rotate(tokens, 1)
    shift_other = swap(side(decay_shift, False), lax.axis_size("tp"), count)
    w_qkv = call(
        pack_kernel, jax.ShapeDtypeStruct((w_query.shape[0], 2 * keys + vals), BF16),
        scal, w_query, w_key, w_value,
    )
    qkv = line_gather(w_qkv)
    w_mix = lax.dynamic_slice_in_dim(w_mix_out, rep * vals, vals, 0)

    gate_in, up_in, down_in, two = lax.optimization_barrier((w_gate, w_up, w_down, qkv[1]))
    qkv = (qkv[0], two, qkv[2])
    qkv_end = line_forward(two)

    def unit_cols(value):
        far = value.shape[1] - main
        return (
            jnp.where(low, value[:, :main], value[:, far:]),
            jnp.where(low, value[:, main:units], value[:, units:far]) if units > main else value[:, :0],
        )

    gate_main, gate_tail = unit_cols(gate_in)
    up_main, up_tail = unit_cols(up_in)
    w_gu = jnp.concatenate([gate_main, up_main, gate_tail, up_tail], axis=1)
    far = down_in.shape[0] - main
    w_dn = jnp.concatenate(
        [
            jnp.where(low, down_in[:main], down_in[far:]),
            jnp.where(low, down_in[main:units], down_in[units:far]),
        ],
        axis=0,
    )
    head = (tp * reps + rep) * keys
    up_cols = lax.dynamic_slice_in_dim(w_decay_up, head, keys, 1)
    bias = lax.dynamic_slice_in_dim(decay_bias, head, keys, 0).reshape(1, keys)
    hgain = lax.dynamic_slice_in_dim(head_gain, (tp * reps + rep) * vals, vals, 0).reshape(1, vals)
    gain_mix = rotate(mix_gain.reshape(1, width), 1)
    gain_ffn = rotate(ffn_gain.reshape(1, width), 1)
    down_cols = rotate(w_decay_down, 0)
    shift_own = side(decay_shift)
    tok, before = plane_gather(
        own_tok, count,
        (w_gu, w_dn, up_cols, bias, hgain, gain_mix, gain_ffn, down_cols, shift_own),
    )
    w_gu, w_dn, up_cols, bias, hgain, gain_mix, gain_ffn, down_cols, shift_own = before
    mix = line_gather(w_mix)
    mix_end = line_forward(mix[1], both=False)
    gu = line_gather(w_gu)
    gu_end = line_forward(gu[1])
    half = w_dn.shape[1] // 2
    near = line_near(w_dn[:, :half]), line_near(w_dn[:, half:])
    two, inner = line_far(w_dn)
    dn_end = line_forward(two)

    struct = jax.ShapeDtypeStruct
    all_rows = count * rows
    proj, logd = call(
        project_kernel,
        [struct((all_rows, 2 * keys + vals), BF16), struct((all_rows, keys), F32)],
        scal, *tok, gain_mix, w_qkv, *qkv, qkv_end, down_cols, up_cols, bias,
        rows=rows,
    )
    gated = call(
        recurrence_kernel, struct((all_rows, vals), BF16),
        scal, proj, logd, shift_own, shift_other, hgain,
        rows=rows, channels=keys, values=vals, blocks=decay_shift.shape[0] // BLK,
    )
    blocks = [struct((count // 2, rows, width), BF16)] * 2
    even, odd = call(mix_kernel, blocks, scal, gated, w_mix, *mix, mix_end, rows=rows)
    mixed = [part.astype(F32) for part in plane_reduce(even, odd, count)]
    hidden = own_tok.astype(F32) + sum(mixed)
    normed = rms_norm(hidden, gain_ffn).astype(BF16)
    pieces, _ = plane_gather(normed, count)
    partial = call(
        gate_first_kernel, struct((all_rows, w_gu.shape[1]), F32),
        scal, *pieces, w_gu, gu[0], gu[1], rows=rows,
    )
    act = call(
        gate_second_kernel, struct((all_rows, units), BF16),
        scal, *pieces, partial, gu[2], gu_end, rows=rows, main=main,
    )
    part = w_dn.shape[1]
    pair = [struct((count // 2, rows, part + half), BF16)] * 2
    single = [struct((count // 2, rows, part), BF16)] * 2
    even, odd = call(columns_kernel, pair, scal, act, w_dn, near[0], rows=rows)
    sum_a = plane_reduce(even, odd, count)
    even, odd = call(columns_kernel, pair, scal, act, two, near[1], rows=rows)
    sum_n = plane_reduce(even, odd, count)
    even, odd = call(second_kernel, single, scal, act, inner, dn_end, rows=rows)
    sum_b = plane_reduce(even, odd, count)
    total = call(merge_kernel, struct((rows, width), F32), scal, hidden, *sum_a, *sum_n, part=part)
    return add_last(scal, total, sum_b)


def layer_device(*args):
    return split_device(*args)


def solution(mesh):
    sizes = dict(mesh.shape)
    fits = sizes["rep"] == 2 and sizes["fs"] == 4 and sizes["tp"] == 4
    per_device = layer_device if fits else plain_device
    return jax.shard_map(
        per_device,
        mesh=mesh,
        in_specs=(
            P(("rep", "fs", "tp"), None),
            P(),
            P("fs", "tp"),
            P("fs", "tp"),
            P("fs", "tp"),
            P(),
            P(),
            P(),
            P(("rep", "fs"), "tp"),
            P(),
            P("tp", "fs"),
            P(),
            P("fs", "tp"),
            P("fs", "tp"),
            P("tp", "fs"),
        ),
        out_specs=P(("rep", "fs", "tp"), None),
        check_vma=False,
    )
```

```python
import functools

import jax
import jax.numpy as jnp
from jax import lax
from jax.experimental import pallas as pl
from jax.experimental.pallas import tpu as pltpu
from jax.sharding import PartitionSpec as P

KEY_CHANNELS = 128
DV = 256
BLK = 64


EPS = 1e-06
TAU = 16.0


def rms_norm(values, gain):
    return values * lax.rsqrt(jnp.mean(values * values, axis=-1, keepdims=True) + EPS) * gain


def recurrence(query_proj, key_proj, value_proj, log_decay, head_count):
    seq_rows = query_proj.shape[0]
    blocks = seq_rows // BLK
    queries = query_proj.astype(jnp.float32).reshape(
        blocks, BLK, head_count, KEY_CHANNELS
    ) * KEY_CHANNELS ** (-0.5)
    keys = key_proj.astype(jnp.float32).reshape(blocks, BLK, head_count, KEY_CHANNELS)
    values = value_proj.astype(jnp.float32).reshape(blocks, BLK, head_count, DV)
    decays = log_decay.reshape(blocks, BLK, head_count, KEY_CHANNELS)
    cumul = jnp.cumsum(decays, axis=1)
    totals = cumul[:, -1]
    weighted = keys * jnp.exp(totals[:, None] - cumul)
    updates = jnp.einsum("bchd,bche->bhde", weighted, values, precision=lax.Precision.HIGHEST)

    def combine(earlier, later):
        return (earlier[0] + later[0], jnp.exp(later[0])[..., None] * earlier[1] + later[1])

    _, states = lax.associative_scan(combine, (totals, updates), axis=0)
    previous = jnp.concatenate([jnp.zeros_like(states[:1]), states[:-1]], axis=0)
    q_decayed = queries * jnp.exp(cumul)
    k_decayed = keys * jnp.exp(-cumul)
    scores = jnp.einsum("bchd,bshd->bhcs", q_decayed, k_decayed, precision=lax.Precision.HIGHEST)
    causal = (jnp.arange(BLK)[:, None] >= jnp.arange(BLK)[None, :]).astype(jnp.float32)
    scores = scores * causal
    inner = jnp.einsum("bhcs,bshe->bche", scores, values, precision=lax.Precision.HIGHEST)
    carried = jnp.einsum("bchd,bhde->bche", q_decayed, previous, precision=lax.Precision.HIGHEST)
    return (inner + carried).reshape(seq_rows, head_count, DV)


def plain_device(
    tokens,
    mix_gain,
    w_query,
    w_key,
    w_value,
    w_decay_down,
    w_decay_up,
    decay_bias,
    decay_shift,
    head_gain,
    w_mix_out,
    ffn_gain,
    w_gate,
    w_up,
    w_down,
):
    tp_index = lax.axis_index("tp")
    own_count = tokens.shape[0]
    key_cols = w_query.shape[1]
    value_cols = w_value.shape[1]
    heads_dev = key_cols // KEY_CHANNELS
    whole_input = lax.all_gather(tokens, "tp", axis=0, tiled=True).astype(jnp.float32)
    normed = rms_norm(whole_input, mix_gain).astype(jnp.bfloat16)
    seq_rows = normed.shape[0]
    pieces = (
        lax.all_gather(w_query, "fs", axis=0, tiled=True),
        lax.all_gather(w_key, "fs", axis=0, tiled=True),
        lax.all_gather(w_value, "fs", axis=0, tiled=True),
    )
    first = jnp.dot(normed, pieces[0], preferred_element_type=jnp.float32)
    second = jnp.dot(normed, pieces[1], preferred_element_type=jnp.float32)
    third = jnp.dot(normed, pieces[2], preferred_element_type=jnp.float32)
    query_proj = first.astype(jnp.bfloat16)
    key_proj = second.astype(jnp.bfloat16)
    value_proj = third.astype(jnp.bfloat16)
    low_rank = jnp.dot(normed, w_decay_down, preferred_element_type=jnp.float32).astype(
        jnp.bfloat16
    )
    up_columns = lax.dynamic_slice_in_dim(w_decay_up, tp_index * key_cols, key_cols, 1)
    bias_columns = lax.dynamic_slice_in_dim(decay_bias, tp_index * key_cols, key_cols, 0)
    pre_decay = jnp.dot(low_rank, up_columns, preferred_element_type=jnp.float32) + bias_columns
    log_decay = jax.nn.log_sigmoid(pre_decay) / TAU + decay_shift
    head_out = recurrence(query_proj, key_proj, value_proj, log_decay, heads_dev)
    gain_columns = lax.dynamic_slice_in_dim(head_gain, tp_index * value_cols, value_cols, 0)
    gated = rms_norm(head_out, gain_columns.reshape(heads_dev, DV)).astype(jnp.bfloat16)
    gated = gated.reshape(seq_rows, value_cols)
    out_weight = lax.all_gather(w_mix_out, "fs", axis=1, tiled=True)
    mixer_full = lax.psum(
        jnp.dot(gated, out_weight, preferred_element_type=jnp.float32).astype(jnp.bfloat16), "tp"
    ).astype(jnp.float32)
    hidden_all = whole_input + mixer_full
    normed_ffn = rms_norm(hidden_all, ffn_gain).astype(jnp.bfloat16)
    hidden = lax.dynamic_slice_in_dim(hidden_all, tp_index * own_count, own_count, 0)

    def add_single(piece):
        return jnp.dot(normed_ffn, piece, preferred_element_type=jnp.float32)

    pieces = (
        lax.all_gather(w_gate, "fs", axis=0, tiled=True),
        lax.all_gather(w_up, "fs", axis=0, tiled=True),
    )
    gate_proj = add_single(pieces[0])
    up_proj = add_single(pieces[1])
    activated = (jax.nn.silu(gate_proj) * up_proj).astype(jnp.bfloat16)
    down_weight = lax.all_gather(w_down, "fs", axis=1, tiled=True)
    return hidden + lax.psum_scatter(
        jnp.dot(activated, down_weight, preferred_element_type=jnp.float32).astype(jnp.bfloat16),
        "tp",
        scatter_dimension=0,
        tiled=True,
    ).astype(jnp.float32)


LANES = 128
F32 = jnp.float32
BF16 = jnp.bfloat16
VMEM = pl.BlockSpec(memory_space=pltpu.VMEM)
SMEM = pl.BlockSpec(memory_space=pltpu.SMEM)
PLANE = ("rep", "tp")


def dot(a, b, dims=((1,), (0,))):
    return lax.dot_general(a, b, (dims, ((), ())), preferred_element_type=F32)


def parts(value):
    high = value.astype(BF16)
    return high, (value - high.astype(F32)).astype(BF16)


def fine_dot(a, b, dims=((1,), (0,))):
    left = (a,) if a.dtype == BF16 else parts(a)
    right = (b,) if b.dtype == BF16 else parts(b)
    total = dot(left[0], right[0], dims)
    if len(right) > 1:
        total = total + dot(left[0], right[1], dims)
    if len(left) > 1:
        total = total + dot(left[1], right[0], dims)
    return total


def swap(value, mask, count):
    return lax.ppermute(value, PLANE, [(i, i ^ mask) for i in range(count)])


def plane_gather(own, count, before=()):
    pieces = [own] + [None] * (count - 1)
    for mask in (4, 2, 6, 1):
        pieces[mask] = swap(own, mask, count)
    if before:
        pieces[6], *before = lax.optimization_barrier((pieces[6], *before))
    for mask in (4, 2, 6):
        pieces[mask + 1] = swap(pieces[mask], 1, count)
    return pieces, before


def plane_reduce(even, odd, count):
    other = swap(odd, 1, count)
    sums = [even[0].astype(F32) + other[0].astype(F32)]
    sent = {
        mask: (even[mask // 2].astype(F32) + other[mask // 2].astype(F32)).astype(BF16)
        for mask in (4, 2, 6)
    }
    return sums + [swap(sent[mask], mask, count) for mask in (6, 4, 2)]


def line_near(own):
    size = lax.axis_size("fs")
    return lax.ppermute(own, "fs", [(i, i ^ 1) for i in range(size)])


def line_far(own):
    size = lax.axis_size("fs")
    two = lax.ppermute(own, "fs", [(i, i ^ 2) for i in range(size)])
    inner = lax.ppermute(own, "fs", [(1, 2), (2, 1)])
    return two, inner


def line_gather(own):
    two, inner = line_far(own)
    return line_near(own), two, inner


def line_forward(two, both=True):
    size = lax.axis_size("fs")
    pairs = [(i, i ^ 1) for i in range(size)] if both else [(1, 0), (2, 3)]
    return lax.ppermute(two, "fs", pairs)


def rotate(value, axis):
    size = lax.axis_size("fs")
    block = value.shape[axis] // size
    index = lax.axis_index("fs")
    order = [index ^ k for k in range(size)]
    return jnp.concatenate(
        [lax.dynamic_slice_in_dim(value, place * block, block, axis) for place in order], axis
    )


def pick_late(scal, inner, fourth):
    at = scal[0]
    return jnp.where(jnp.logical_or(at == 0, at == 3), fourth[...], inner[...])


def pick_weights(scal, own_w, near, two, inner, fourth):
    return [own_w[...], near[...], two[...], pick_late(scal, inner, fourth)]


def project_kernel(scal, *refs, rows):
    tok = refs[:8]
    gain, own_w, near, two, inner, fourth, down_w, up_w, bias, proj, logd = refs[8:]
    weight = pick_weights(scal, own_w, near, two, inner, fourth)
    part = own_w.shape[0]
    for m in range(8):
        source = tok[m][...].astype(F32)
        scale = lax.rsqrt(jnp.mean(source * source, axis=-1, keepdims=True) + EPS)
        normed = (source * scale * gain[...]).astype(BF16)
        total = dot(normed[:, :part], weight[0])
        for k in range(1, 4):
            total = total + dot(normed[:, k * part : (k + 1) * part], weight[k])
        proj[m * rows : (m + 1) * rows, :] = total.astype(BF16)
        low = dot(normed, down_w[...]).astype(BF16)
        pre = dot(low, up_w[...]) + bias[...]
        logd[m * rows : (m + 1) * rows, :] = jax.nn.log_sigmoid(pre) / TAU


def recurrence_kernel(
    scal, proj, logd, shift_own, shift_other, hgain, gated_out, *, rows, channels, values, blocks
):
    place = scal[1]
    tri_row = lax.broadcasted_iota(jnp.int32, (BLK, BLK), 0)
    tri_col = lax.broadcasted_iota(jnp.int32, (BLK, BLK), 1)
    tri = (tri_row >= tri_col).astype(F32)
    per = rows // BLK
    states = [None, None]
    for b in range(blocks):
        for seq in range(2):
            shift = (shift_own, shift_other)[seq]
            m = seq * 4 + ((b // per) ^ place)
            offset = pl.multiple_of(m * rows + (b % per) * BLK, BLK)
            decay = logd[pl.ds(offset, BLK), :] + shift[b * BLK : (b + 1) * BLK, :]
            cum = lax.dot_general(
                tri, decay, (((1,), (0,)), ((), ())),
                precision=lax.Precision.HIGHEST, preferred_element_type=F32,
            )
            tot = cum[BLK - 1 :, :]
            q = proj[pl.ds(offset, BLK), :channels].astype(F32) * channels ** (-0.5)
            k = proj[pl.ds(offset, BLK), channels : 2 * channels].astype(F32)
            v = proj[pl.ds(offset, BLK), 2 * channels :]
            qd = q * jnp.exp(cum)
            kd = k * jnp.exp(-cum)
            scores = lax.dot_general(
                qd, kd, (((1,), (1,)), ((), ())),
                precision=lax.Precision.HIGHEST, preferred_element_type=F32,
            )
            out = fine_dot(scores * tri, v)
            if b:
                out = out + fine_dot(qd, states[seq], ((1,), (1,)))
            scale = lax.rsqrt(jnp.mean(out * out, axis=-1, keepdims=True) + EPS)
            gated_out[pl.ds(offset, BLK), :] = (out * scale * hgain[...]).astype(BF16)
            if b + 1 < blocks:
                update = fine_dot(v, k * jnp.exp(tot - cum), ((0,), (0,)))
                states[seq] = jnp.exp(tot) * states[seq] + update if b else update


def store_blocks(value, weights, even, odd, rows):
    for m in range(8):
        left = value[m * rows : (m + 1) * rows, :]
        out = (even, odd)[m % 2]
        start = 0
        for weight in weights:
            size = weight.shape[1]
            out[m // 2, :, start : start + size] = dot(left, weight).astype(BF16)
            start += size


def mix_kernel(scal, value, own_w, near, two, inner, fourth, even, odd, *, rows):
    store_blocks(value, pick_weights(scal, own_w, near, two, inner, fourth), even, odd, rows)


def columns_kernel(scal, value, *refs, rows):
    *weights, even, odd = refs
    store_blocks(value, [weight[...] for weight in weights], even, odd, rows)


def second_kernel(scal, value, inner, fourth, even, odd, *, rows):
    store_blocks(value, [pick_late(scal, inner, fourth)], even, odd, rows)


def gate_first_kernel(scal, *refs, rows):
    pieces = refs[:8]
    own_w, near, two, total = refs[8:]
    part = own_w.shape[0]
    for m in range(8):
        value = dot(pieces[m][:, :part], own_w[...])
        value = value + dot(pieces[m][:, part : 2 * part], near[...])
        value = value + dot(pieces[m][:, 2 * part : 3 * part], two[...])
        total[m * rows : (m + 1) * rows, :] = value


def gate_second_kernel(scal, *refs, rows, main):
    pieces = refs[:8]
    partial, inner, fourth, act = refs[8:]
    weight = pick_late(scal, inner, fourth)
    tail = weight.shape[1] // 2 - main
    for m in range(8):
        place = slice(m * rows, (m + 1) * rows)
        total = partial[place, :] + dot(pieces[m][...], weight)
        act[place, :main] = (jax.nn.silu(total[:, :main]) * total[:, main : 2 * main]).astype(BF16)
        if tail:
            gate = total[:, 2 * main : 2 * main + tail]
            act[place, main:] = (jax.nn.silu(gate) * total[:, 2 * main + tail :]).astype(BF16)


def pack_kernel(scal, query, key, value, out):
    start = 0
    for ref in (query, key, value):
        size = ref.shape[1] // 2
        from_col = pl.multiple_of(scal[2] * size, LANES)
        out[:, start : start + size] = ref[:, pl.ds(from_col, size)]
        start += size


def merge_kernel(scal, hidden, *refs, part):
    *groups, out = refs
    at = scal[0]
    half = part // 2
    place = {0: [(0, 0, part)], 1: [(0, part, half), (1, part, half)], 2: [(1, 0, part)], 3: []}
    for k, pieces in place.items():
        total = hidden[:, k * part : (k + 1) * part]
        if pieces:
            total = total + jnp.concatenate(
                [
                    sum(ref[:, col : col + size].astype(F32) for ref in groups[4 * g : 4 * g + 4])
                    for g, col, size in pieces
                ],
                axis=1,
            )
        out[:, pl.ds(pl.multiple_of((at ^ k) * part, part), part)] = total


def call(kernel, outs, *args, specs=(), **static):
    return pl.pallas_call(
        functools.partial(kernel, **static),
        grid=(1,) if specs else (),
        out_shape=outs,
        in_specs=[SMEM, *specs] + [VMEM] * (len(args) - 1 - len(specs)),
        out_specs=jax.tree.map(lambda _: VMEM, outs),
        compiler_params=pltpu.CompilerParams(vmem_limit_bytes=60 * 1024 * 1024),
    )(*args)


def split_device(
    tokens,
    mix_gain,
    w_query,
    w_key,
    w_value,
    w_decay_down,
    w_decay_up,
    decay_bias,
    decay_shift,
    head_gain,
    w_mix_out,
    ffn_gain,
    w_gate,
    w_up,
    w_down,
):
    rep, at, tp = (lax.axis_index(name) for name in ("rep", "fs", "tp"))
    reps = lax.axis_size("rep")
    count = reps * lax.axis_size("tp")
    rows, width = tokens.shape
    low = rep == 0
    keys, vals = w_query.shape[1] // reps, w_value.shape[1] // reps
    units = w_gate.shape[1] // reps
    main = units // LANES * LANES
    scal = jnp.stack([at, tp, rep]).astype(jnp.int32)

    def side(value, own=True):
        half = value.shape[1] // 2
        pick = low if own else jnp.logical_not(low)
        return jnp.where(pick, value[:, :half], value[:, half:])

    own_tok = rotate(tokens, 1)
    shift_other = swap(side(decay_shift, False), lax.axis_size("tp"), count)
    w_qkv = call(
        pack_kernel, jax.ShapeDtypeStruct((w_query.shape[0], 2 * keys + vals), BF16),
        scal, w_query, w_key, w_value,
    )
    qkv = line_gather(w_qkv)
    w_mix = lax.dynamic_slice_in_dim(w_mix_out, rep * vals, vals, 0)

    gate_in, up_in, down_in, two = lax.optimization_barrier((w_gate, w_up, w_down, qkv[1]))
    qkv = (qkv[0], two, qkv[2])
    qkv_end = line_forward(two)

    def unit_cols(value):
        far = value.shape[1] - main
        return (
            jnp.where(low, value[:, :main], value[:, far:]),
            jnp.where(low, value[:, main:units], value[:, units:far]) if units > main else value[:, :0],
        )

    gate_main, gate_tail = unit_cols(gate_in)
    up_main, up_tail = unit_cols(up_in)
    w_gu = jnp.concatenate([gate_main, up_main, gate_tail, up_tail], axis=1)
    far = down_in.shape[0] - main
    w_dn = jnp.concatenate(
        [
            jnp.where(low, down_in[:main], down_in[far:]),
            jnp.where(low, down_in[main:units], down_in[units:far]),
        ],
        axis=0,
    )
    head = (tp * reps + rep) * keys
    up_cols = lax.dynamic_slice_in_dim(w_decay_up, head, keys, 1)
    bias = lax.dynamic_slice_in_dim(decay_bias, head, keys, 0).reshape(1, keys)
    hgain = lax.dynamic_slice_in_dim(head_gain, (tp * reps + rep) * vals, vals, 0).reshape(1, vals)
    gain_mix = rotate(mix_gain.reshape(1, width), 1)
    gain_ffn = rotate(ffn_gain.reshape(1, width), 1)
    down_cols = rotate(w_decay_down, 0)
    shift_own = side(decay_shift)
    tok, before = plane_gather(
        own_tok, count,
        (w_gu, w_dn, up_cols, bias, hgain, gain_mix, gain_ffn, down_cols, shift_own),
    )
    w_gu, w_dn, up_cols, bias, hgain, gain_mix, gain_ffn, down_cols, shift_own = before
    mix = line_gather(w_mix)
    mix_end = line_forward(mix[1], both=False)
    gu = line_gather(w_gu)
    gu_end = line_forward(gu[1])
    half = w_dn.shape[1] // 2
    near = line_near(w_dn[:, :half]), line_near(w_dn[:, half:])
    two, inner = line_far(w_dn)
    dn_end = line_forward(two)

    struct = jax.ShapeDtypeStruct
    all_rows = count * rows
    proj, logd = call(
        project_kernel,
        [struct((all_rows, 2 * keys + vals), BF16), struct((all_rows, keys), F32)],
        scal, *tok, gain_mix, w_qkv, *qkv, qkv_end, down_cols, up_cols, bias,
        rows=rows,
    )
    gated = call(
        recurrence_kernel, struct((all_rows, vals), BF16),
        scal, proj, logd, shift_own, shift_other, hgain,
        rows=rows, channels=keys, values=vals, blocks=decay_shift.shape[0] // BLK,
    )
    blocks = [struct((count // 2, rows, width), BF16)] * 2
    even, odd = call(mix_kernel, blocks, scal, gated, w_mix, *mix, mix_end, rows=rows)
    mixed = [part.astype(F32) for part in plane_reduce(even, odd, count)]
    hidden = own_tok.astype(F32) + sum(mixed)
    normed = rms_norm(hidden, gain_ffn).astype(BF16)
    pieces, _ = plane_gather(normed, count)
    partial = call(
        gate_first_kernel, struct((all_rows, w_gu.shape[1]), F32),
        scal, *pieces, w_gu, gu[0], gu[1], rows=rows,
        specs=[pl.BlockSpec((rows, 3 * w_gu.shape[0]), lambda i: (0, 0))] * count,
    )
    act = call(
        gate_second_kernel, struct((all_rows, units), BF16),
        scal, *pieces, partial, gu[2], gu_end, rows=rows, main=main,
        specs=[pl.BlockSpec((rows, w_gu.shape[0]), lambda i: (0, 3))] * count,
    )
    part = w_dn.shape[1]
    pair = [struct((count // 2, rows, part + half), BF16)] * 2
    single = [struct((count // 2, rows, part), BF16)] * 2
    even, odd = call(columns_kernel, pair, scal, act, w_dn, near[0], rows=rows)
    sum_a = plane_reduce(even, odd, count)
    even, odd = call(columns_kernel, pair, scal, act, two, near[1], rows=rows)
    sum_n = plane_reduce(even, odd, count)
    even, odd = call(second_kernel, single, scal, act, inner, dn_end, rows=rows)
    sum_b = plane_reduce(even, odd, count)
    total = call(merge_kernel, struct((rows, width), F32), scal, hidden, *sum_a, *sum_n, part=part)
    where = (at ^ 3) * part
    late = lax.dynamic_slice_in_dim(total, where, part, 1)
    late = late + sum(value.astype(F32) for value in sum_b)
    return lax.dynamic_update_slice_in_dim(total, late, where, 1)


def layer_device(*args):
    return split_device(*args)


def solution(mesh):
    sizes = dict(mesh.shape)
    fits = sizes["rep"] == 2 and sizes["fs"] == 4 and sizes["tp"] == 4
    per_device = layer_device if fits else plain_device
    return jax.shard_map(
        per_device,
        mesh=mesh,
        in_specs=(
            P(("rep", "fs", "tp"), None),
            P(),
            P("fs", "tp"),
            P("fs", "tp"),
            P("fs", "tp"),
            P(),
            P(),
            P(),
            P(("rep", "fs"), "tp"),
            P(),
            P("tp", "fs"),
            P(),
            P("fs", "tp"),
            P("fs", "tp"),
            P("tp", "fs"),
        ),
        out_specs=P(("rep", "fs", "tp"), None),
        check_vma=False,
    )
```
